32 devices in a mesh: ep: 8 (over z, x), tp: 4 (over y, core).
Axes of the slice: x: 2, y: 2, z: 4, core: 2. Of those that a mesh axis runs over, the one named last changes fastest.
Arguments:
- queries: bfloat16 [1024, 1024], P('ep', 'tp'), may hold values from -6 to 6
- key_states: bfloat16 [1024, 256], P('ep'), may hold values from -192 to 192
- value_states: bfloat16 [1024, 256], P('ep'), may hold values from -12 to 12
- sink_logit: float32 [16], P('tp'), may hold values from 3 to 7
- out_weight: bfloat16 [1024, 2048], P('tp'), may hold values from -0.1875 to 0.1875
- expert_input: bfloat16 [1024, 2048], P('ep'), may hold values from -6 to 6
- norm_gain: float32 [2048], replicated, may hold values from 0.1 to 1.9
- routes: int32 [1024, 2], P('ep'), may hold values from 0 to 7, all different within a row; in each aligned block of 128 rows (0 to 127, 128 to 255, ...) at most 40 rows name the same one
- route_weight: float32 [1024, 2], P('ep'), may hold values from 0.1 to 1
- gate_weight: bfloat16 [8, 2048, 4096], P('ep', None, 'tp'), may hold values from -0.125 to 0.125
- up_weight: bfloat16 [8, 2048, 4096], P('ep', None, 'tp'), may hold values from -0.125 to 0.125
- down_weight: bfloat16 [8, 4096, 2048], P('ep', 'tp'), may hold values from -0.125 to 0.125
Outputs:
- mixer_out: bfloat16 [1024, 2048], P(('ep', 'tp'))
- expert_out: bfloat16 [1024, 2048], P('ep', 'tp')
The draws below stay inside these ranges and needn't reach their ends.
Inputs may be any that keep to these rules, and one draw needn't show every extreme that they name: `routes`: each row names 2 different experts. Within the rows of one index of ep (aligned blocks of 128 rows) no expert is named more than 40 times, a bound that some blocks reach.
All inputs are finite; a program needn't handle non-finite values.
Results may differ from the reference program's by a relative error of at most 0.025.
Values may be sent and summed in bfloat16 or wider, within the bound.
No kernel may reach another device: no remote copies, remote signals or barrier semaphores. Data moves between devices by JAX's collectives and lax.ppermute only.
A program may use at most 64 MiB of HBM per device.

```python
import math
import jax
import jax.numpy as jnp
import numpy as np
from jax import lax

D = 2048
HEADS = 16
KV_HEADS = 4
HEAD_DIM = 64
FF = 4096
WINDOW = 128
TOP = 2
TOK_DEV = 128
TOKENS = 1024
EXPERTS = 8
CAP = 40
HEADS_DEV = 4
FF_DEV = 1024
N_EP = 8
N_TP = 4


def draw_key_states(key, part):
    normal_draw = jax.random.truncated_normal(key, -4.0, 4.0, (TOKENS, KV_HEADS * HEAD_DIM), jnp.float32)
    return normal_draw.astype(jnp.bfloat16)


def spiked(array, own_key, source, target, blocks, factor):
    def block_of(position):
        return (jnp.arange(array.shape[position]) // (array.shape[position] // blocks)).reshape((-1,) + (1,) * (array.ndim - 1 - position))

    first = jax.random.permutation(own_key, blocks)[block_of(target)]
    other_side = (block_of(target) + blocks // 2) % blocks
    return jnp.where((block_of(source) == first) | (block_of(source) == other_side), factor * array, array)


def level_of(key, extent, split, least, top_value):
    level = 1.0
    for position, parts in split:
        steps = jax.random.uniform(jax.random.fold_in(jax.random.fold_in(key, 6), position), (parts,), jnp.float32, least / len(split), top_value / len(split))
        level = level * jnp.repeat(jnp.exp(steps), extent[position] // parts).reshape((-1,) + (1,) * (len(extent) - 1 - position))
    return level


def deal_out(rng, own, number, rows, amount, top, limit, skew):
    sequence = jax.random.permutation(rng, amount)
    crowded, common = shares(amount, rows * top, limit, skew, True), shares(amount, rows * top, limit, skew, False)
    places = jnp.arange(amount)

    def named(lengths, rotation):
        used = int((lengths > 0).sum())
        fixed = max(1, used // 4)
        shifted = fixed + (places - fixed + rotation * (used - fixed)) % max(1, amount - fixed)
        return jnp.zeros((amount,), jnp.int32).at[sequence[jnp.where(places < fixed, places, shifted)]].set(jnp.asarray(lengths, jnp.int32))

    lengths = jnp.where(number % 4 == 0, named(crowded, number // 4), named(common, number - number // 4 - 1))
    mixed = jax.random.permutation(jax.random.fold_in(own, 3), amount)
    source_of, receiver = mixed[0:amount // 2 * 2:2], mixed[1:amount // 2 * 2:2]
    slack = jnp.minimum(lengths[source_of] - 1, limit - lengths[receiver]) // 2
    slack = jnp.where((source_of == sequence[0]) | (receiver == sequence[0]) | (lengths[receiver] == 0), 0, jnp.maximum(slack, 0))
    shifted = jax.random.randint(jax.random.fold_in(own, 4), (amount // 2,), 0, 1 << 20) % (slack + 1)
    lengths = lengths.at[source_of].add(-shifted).at[receiver].add(shifted)
    labels = jnp.searchsorted(jnp.cumsum(lengths), jnp.arange(rows * top), side="right").astype(jnp.int32)
    grid = labels.reshape(top, rows).T
    grid = grid[jax.random.permutation(jax.random.fold_in(own, 1), rows)]
    rotation = jax.random.randint(jax.random.fold_in(own, 2), (rows, 1), 0, top)
    return jnp.take_along_axis(grid, (jnp.arange(top)[None, :] + rotation) % top, axis=1)


def shares(amount, total, reach, slope, full):
    weights = [(1 << 20) // math.isqrt(grade ** slope) + 1 for grade in range(1, amount + 1)]
    largest = reach if full else min(reach, max(-(-total // amount), total * weights[0] // sum(weights)))
    least = 1 if total - largest >= amount - 1 else 0
    counts, rest = [largest] + [least] * (amount - 1), total - largest - least * (amount - 1)
    while rest > 0:
        free = [i for i in range(1, amount) if counts[i] < largest] or [i for i in range(1, amount) if counts[i] < reach]
        pool, remaining = sum([weights[i] for i in free]), rest
        for i in free:
            more = min(reach - counts[i], max(1, remaining * weights[i] // pool), rest)
            counts[i] = counts[i] + more
            rest = rest - more
    return np.array(counts)


def normal_values(stream_key, dims, scale, limit, shards=(), held_as=jnp.bfloat16):
    factor_of = level_of(stream_key, dims, shards, -0.22, 0.18) if shards else 1.0
    array = jax.random.normal(stream_key, dims, jnp.float32) * scale * factor_of
    return jnp.minimum(jnp.maximum(array, -limit), limit).astype(held_as)


def noise_with(own_key, extent, scale, limit, shards, heavy, held_as=jnp.bfloat16):
    entries = scale * jax.random.normal(own_key, extent, jnp.float32)
    if shards:
        entries = entries * level_of(own_key, extent, shards, -0.22, 0.18)
    return jnp.clip(spiked(entries, jax.random.fold_in(own_key, 3), *heavy), -limit, limit).astype(held_as)


def setup_inputs(seed: int = 0) -> dict:
    keys = jax.random.split(jax.random.key(seed), 13)
    queries = normal_values(keys[0], (TOKENS, HEADS * HEAD_DIM), 1.0, 6.0, ((0, 8), (1, 4)))
    key_states = draw_key_states(jax.random.fold_in(keys[12], 71), 0)
    value_states = normal_values(keys[2], (TOKENS, KV_HEADS * HEAD_DIM), 2.0, 12.0, ((0, 8),))
    sink_logit = jnp.clip(3.0 + 4.0 * jax.random.uniform(keys[3], (HEADS,), jnp.float32) ** level_of(keys[3], (HEADS,), ((0, 4),), -0.2, 0.2), 3.0, 7.0)
    out_weight = normal_values(keys[4], (HEADS * HEAD_DIM, D), (HEADS * HEAD_DIM) ** -0.5, 0.1875, ((0, 4),))
    expert_input = normal_values(keys[5], (TOKENS, D), 1.0, 6.0, ((0, 8),))
    norm_gain = jnp.clip(1.0 + 0.18 * jax.random.normal(keys[6], (D,), jnp.float32), 0.1, 1.9)
    routes_keys = jax.random.split(jax.random.fold_in(keys[7], 1), TOKENS // TOK_DEV)
    routes_turns = jax.random.permutation(jax.random.fold_in(keys[7], 3), TOKENS // TOK_DEV)
    routes = jax.vmap(lambda own, number: deal_out(jax.random.fold_in(keys[7], 2), own, number, TOK_DEV, EXPERTS, TOP, CAP, 1))(routes_keys, routes_turns).reshape((TOKENS, TOP))
    route_weight = jnp.clip(0.1 + 0.9 * jax.random.uniform(keys[8], (TOKENS, TOP), jnp.float32) ** level_of(keys[8], (TOKENS, TOP), ((0, 8),), -0.2, 0.2), 0.1, 1.0)
    gate_weight = normal_values(keys[9], (EXPERTS, D, FF), D ** -0.5, 0.125, ((0, 8), (2, 4)))
    up_weight = normal_values(keys[10], (EXPERTS, D, FF), D ** -0.5, 0.125, ((0, 8), (2, 4)))
    down_weight = noise_with(keys[11], (EXPERTS, FF, D), FF ** -0.5, 0.125, ((0, 8), (1, 4)), (1, 2, 4, 2.0))
    return dict(queries=queries, key_states=key_states, value_states=value_states, sink_logit=sink_logit, out_weight=out_weight, expert_input=expert_input, norm_gain=norm_gain, routes=routes, route_weight=route_weight, gate_weight=gate_weight, up_weight=up_weight, down_weight=down_weight)


NORM_EPSILON = 1e-05
ROTARY_BASE = 500000.0
MASK_VALUE = -1e+30

def layer_norm(activations, norm_gain):
    values = activations.astype(jnp.float32)
    average = lax.optimization_barrier(jnp.mean(values, axis=-1, keepdims=True))
    centred = values - average
    variance = lax.optimization_barrier(jnp.mean(centred * centred, axis=-1, keepdims=True))
    return (centred * lax.rsqrt(variance + NORM_EPSILON) * norm_gain).astype(jnp.bfloat16)

def rotate(head_rows, positions):
    half_dim = head_rows.shape[-1] // 2
    exponent = jnp.arange(half_dim, dtype=jnp.float32) * (2.0 / head_rows.shape[-1])
    frequency = jnp.power(jnp.float32(ROTARY_BASE), -exponent)
    angles = positions.astype(jnp.float32)[:, None] * frequency[None, :]
    cosine = jnp.cos(angles)[:, None, :]
    sine_part = jnp.sin(angles)[:, None, :]
    first_half = head_rows[..., :half_dim].astype(jnp.float32)
    second_half = head_rows[..., half_dim:].astype(jnp.float32)
    turned = jnp.concatenate([first_half * cosine - second_half * sine_part, second_half * cosine + first_half * sine_part], axis=-1)
    return turned.astype(jnp.bfloat16)

def attention(queries, key_states, value_states, sink_logit):
    token_count = queries.shape[0]
    group_size = HEADS // KV_HEADS
    positions = jnp.arange(token_count, dtype=jnp.int32)
    turned_query = rotate(queries.reshape(token_count, HEADS, HEAD_DIM), positions)
    turned_key = rotate(key_states.reshape(token_count, KV_HEADS, HEAD_DIM), positions)
    padding = jnp.zeros((WINDOW, KV_HEADS, HEAD_DIM), jnp.bfloat16)
    padded_key = jnp.concatenate([padding, turned_key, padding], axis=0)
    padded_value = jnp.concatenate([padding, value_states.reshape(token_count, KV_HEADS, HEAD_DIM), padding], axis=0)
    span_length = TOK_DEV + 2 * WINDOW
    sinks = sink_logit.astype(jnp.float32).reshape(KV_HEADS, group_size)[:, :, None, None]

    def attend(block_index):
        offset = block_index * TOK_DEV
        block_query = lax.dynamic_slice_in_dim(turned_query, offset, TOK_DEV, 0)
        block_query = block_query.reshape(TOK_DEV, KV_HEADS, group_size, HEAD_DIM).astype(jnp.float32)
        block_key = lax.dynamic_slice_in_dim(padded_key, offset, span_length, 0).astype(jnp.float32)
        block_value = lax.dynamic_slice_in_dim(padded_value, offset, span_length, 0).astype(jnp.float32)
        scores = jnp.einsum('qkgd,skd->kgqs', block_query, block_key) * HEAD_DIM ** (-0.5)
        query_pos = offset + jnp.arange(TOK_DEV, dtype=jnp.int32)[:, None]
        key_pos = offset - WINDOW + jnp.arange(span_length, dtype=jnp.int32)[None, :]
        allowed = (jnp.abs(query_pos - key_pos) <= WINDOW) & (key_pos >= 0) & (key_pos < token_count)
        scores = jnp.where(allowed, scores, MASK_VALUE)
        largest = jnp.maximum(lax.optimization_barrier(jnp.max(scores, axis=-1, keepdims=True)), sinks)
        weights = jnp.exp(scores - largest)
        denominator = lax.optimization_barrier(jnp.sum(weights, axis=-1, keepdims=True)) + jnp.exp(sinks - largest)
        probability = lax.optimization_barrier((weights / denominator).astype(jnp.bfloat16))
        attended = jnp.einsum('kgqs,skd->qkgd', probability.astype(jnp.float32), block_value)
        return attended.astype(jnp.bfloat16).reshape(TOK_DEV, HEADS * HEAD_DIM)
    blocks = lax.map(attend, jnp.arange(token_count // TOK_DEV, dtype=jnp.int32))
    return blocks.reshape(token_count, HEADS * HEAD_DIM)

def reference(queries, key_states, value_states, sink_logit, out_weight, expert_input, norm_gain, routes, route_weight, gate_weight, up_weight, down_weight):
    attended = attention(queries, key_states, value_states, sink_logit)
    column_count = HEADS_DEV * HEAD_DIM

    def add_group(running, group_index):
        part_rows = lax.dynamic_slice_in_dim(attended, group_index * column_count, column_count, 1)
        part_weight = lax.dynamic_slice_in_dim(out_weight, group_index * column_count, column_count, 0)
        partial_value = jnp.dot(part_rows, part_weight, preferred_element_type=jnp.float32).astype(jnp.bfloat16)
        partial_value = lax.optimization_barrier(partial_value)
        return (running + partial_value.astype(jnp.float32), None)
    mixer_total, _ = lax.scan(add_group, jnp.zeros((TOKENS, D), jnp.float32), jnp.arange(N_TP, dtype=jnp.int32))
    mixer_out = mixer_total.astype(jnp.bfloat16)
    normed = layer_norm(expert_input, norm_gain)
    assign_count = TOK_DEV * TOP
    expert_ids = routes.reshape(N_EP, assign_count)
    matches = (expert_ids[:, :, None] == jnp.arange(EXPERTS, dtype=jnp.int32)[None, None, :]).astype(jnp.int32)
    slot_rank = lax.optimization_barrier(jnp.sum((jnp.cumsum(matches, axis=1) - matches) * matches, axis=2))
    slot_index = jnp.arange(N_EP, dtype=jnp.int32)[:, None] * CAP + slot_rank
    token_ids = jnp.arange(N_EP, dtype=jnp.int32)[:, None] * TOK_DEV + jnp.arange(assign_count, dtype=jnp.int32)[None, :] // TOP
    slot_rows = N_EP * CAP
    flat_place = (expert_ids * slot_rows + slot_index).reshape(-1)
    slot_token = jnp.zeros((EXPERTS * slot_rows,), jnp.int32).at[flat_place].set(token_ids.reshape(-1))
    slot_token = slot_token.reshape(EXPERTS, slot_rows)

    def run_expert(expert_id):
        gathered = jnp.take(normed, slot_token[expert_id], axis=0)
        gate_act = jnp.dot(gathered, gate_weight[expert_id], preferred_element_type=jnp.float32)
        up_act = jnp.dot(gathered, up_weight[expert_id], preferred_element_type=jnp.float32)
        hidden = (jax.nn.silu(gate_act) * up_act).astype(jnp.bfloat16)
        hidden_parts = hidden.reshape(slot_rows, N_TP, FF_DEV).astype(jnp.float32)
        down_parts = down_weight[expert_id].reshape(N_TP, FF_DEV, D).astype(jnp.float32)
        partial_value = jnp.einsum('rjf,jfd->jrd', hidden_parts, down_parts).astype(jnp.bfloat16)
        partial_value = lax.optimization_barrier(partial_value)
        return lax.optimization_barrier(jnp.sum(partial_value.astype(jnp.float32), axis=0)).astype(jnp.bfloat16)
    results = lax.map(run_expert, jnp.arange(EXPERTS, dtype=jnp.int32))
    picked = results[expert_ids, slot_index].reshape(TOKENS, TOP, D).astype(jnp.float32)
    rounded_weight = lax.optimization_barrier(route_weight.astype(jnp.bfloat16)).astype(jnp.float32)
    expert_out = lax.optimization_barrier(jnp.sum(rounded_weight[:, :, None] * picked, axis=1)).astype(jnp.bfloat16)
    return (mixer_out, expert_out)
```

```python
import functools

import jax
import jax.numpy as jnp
from jax import lax
from jax.experimental import pallas as pl
from jax.experimental.pallas import tpu as pltpu
from jax.sharding import PartitionSpec as P

HEADS = 16
KV_HEADS = 4
HEAD_DIM = 64
WINDOW = 128
TOP = 2

NORM_EPSILON = 1e-05
ROTARY_BASE = 500000.0
MASK_VALUE = -1e30
LANES = 128
MIB = 1 << 20

VM = pl.BlockSpec(memory_space=pltpu.VMEM)
SM = pl.BlockSpec(memory_space=pltpu.SMEM)
ANY = pl.BlockSpec(memory_space=pl.ANY)
BF = jnp.bfloat16
F32 = jnp.float32


def call(body, out_shape, operands, in_specs, scratch=(), flops=0, nbytes=0, limit=24, out_specs=None, name=None):
    return pl.pallas_call(
        body,
        out_shape=out_shape,
        in_specs=in_specs,
        out_specs=out_specs if out_specs is not None else [VM] * len(out_shape),
        scratch_shapes=list(scratch),
        cost_estimate=pl.CostEstimate(flops=flops, bytes_accessed=nbytes, transcendentals=0),
        compiler_params=pltpu.CompilerParams(vmem_limit_bytes=limit * MIB),
        name=name,
    )(*operands)


def iota(shape, dim):
    return lax.broadcasted_iota(jnp.int32, shape, dim)


def strict_lower(n):
    return (iota((n, n), 0) > iota((n, n), 1)).astype(BF)


def matmul(a, b, dims=(((1,), (0,)), ((), ()))):
    return lax.dot_general(a, b, dims, preferred_element_type=F32)


def pack_body(cap, hops, group, place_ref, x_ref, gain_ref, routes_ref, key_ref, value_ref, kv_ref, *block_refs):
    ep_index, tp_index, head = place_ref[0], place_ref[1], place_ref[2]
    rows = x_ref.shape[0]
    keys, values = key_ref[...], value_ref[...]
    own_key = jnp.zeros((rows, HEAD_DIM), BF)
    own_value = jnp.zeros((rows, HEAD_DIM), BF)
    for h in range(keys.shape[1] // HEAD_DIM):
        own_key = jnp.where(head == h, keys[:, h * HEAD_DIM : (h + 1) * HEAD_DIM], own_key)
        own_value = jnp.where(head == h, values[:, h * HEAD_DIM : (h + 1) * HEAD_DIM], own_value)
    kv_ref[:, :HEAD_DIM] = own_key
    kv_ref[:, HEAD_DIM:] = own_value

    x = x_ref[...].astype(F32)
    average = jnp.mean(x, axis=-1, keepdims=True)
    centred = x - average
    variance = jnp.mean(centred * centred, axis=-1, keepdims=True)
    normed = (centred * lax.rsqrt(variance + NORM_EPSILON) * gain_ref[...]).astype(BF)

    pitch = LANES // hops
    column = iota((1, LANES), 1)
    hop, slot = column // pitch, column % pitch
    target = ep_index ^ (hop * group + tp_index)
    target = jnp.where(slot < cap, target, -1)
    hit = (routes_ref[:, 0:1] == target) | (routes_ref[:, 1:2] == target)
    rank = matmul(strict_lower(rows), hit.astype(BF))
    pick = jnp.where(hit & (rank.astype(jnp.int32) == slot), 1.0, 0.0)
    sent = matmul(jnp.transpose(pick).astype(BF), normed)
    for k, block_ref in enumerate(block_refs):
        block_ref[...] = sent[k * pitch : k * pitch + cap].astype(BF)


def mixer_body(
    cap, order, place_ref, q_ref, kv_ref, low_ref, high_ref, table_ref, sink_ref, routes_ref, rw_ref,
    wo_ref, wg_ref, wu_ref, wd_ref,
    send_ref, keep_ref, combine_ref, vg_ref, vu_ref, vd_ref, att_ref, sems,
):
    copies = [
        pltpu.make_async_copy(wg_ref, vg_ref, sems.at[0]),
        pltpu.make_async_copy(wu_ref, vu_ref, sems.at[1]),
        pltpu.make_async_copy(wd_ref, vd_ref, sems.at[2]),
    ]
    for c in copies:
        c.start()
    ep_index, tp_index = place_ref[0], place_ref[1]
    ep_count = place_ref[3]
    rows = q_ref.shape[0]
    span = rows + 2 * WINDOW
    heads = q_ref.shape[1] // HEAD_DIM
    half = HEAD_DIM // 2
    swap = (iota((HEAD_DIM, HEAD_DIM), 0) == (iota((HEAD_DIM, HEAD_DIM), 1) + half) % HEAD_DIM).astype(BF)
    table = table_ref[...]
    cosine, sine = table[:, :HEAD_DIM], table[:, HEAD_DIM:]
    kv = jnp.concatenate([low_ref[...], kv_ref[...], high_ref[...]], axis=0)
    raw_key, span_value = kv[:, :HEAD_DIM], kv[:, HEAD_DIM:]
    span_key = (raw_key.astype(F32) * cosine + matmul(raw_key, swap) * sine).astype(BF)
    own_cosine, own_sine = cosine[WINDOW : WINDOW + rows], sine[WINDOW : WINDOW + rows]
    distance = iota((rows, span), 1) - WINDOW - iota((rows, span), 0)
    key_pos = ep_index * rows - WINDOW + iota((rows, span), 1)
    allowed = (jnp.abs(distance) <= WINDOW) & (key_pos >= 0) & (key_pos < rows * ep_count)
    for h in range(heads):
        q = q_ref[:, h * HEAD_DIM : (h + 1) * HEAD_DIM]
        q = (q.astype(F32) * own_cosine + matmul(q, swap) * own_sine).astype(BF)
        scores = matmul(q, span_key, (((1,), (1,)), ((), ()))) * HEAD_DIM ** (-0.5)
        scores = jnp.where(allowed, scores, MASK_VALUE)
        sink = sink_ref[h]
        largest = jnp.maximum(jnp.max(scores, axis=-1, keepdims=True), sink)
        weights = jnp.exp(scores - largest)
        total = jnp.sum(weights, axis=-1, keepdims=True) + jnp.exp(sink - largest)
        probability = (weights / total).astype(BF)
        att_ref[:, h * HEAD_DIM : (h + 1) * HEAD_DIM] = matmul(probability, span_value)
    share = rows // len(order)
    piece = lambda n: att_ref[pl.ds(pl.multiple_of((tp_index ^ n) * share, share), share), :]
    ordered = jnp.concatenate([piece(n) for n in order], axis=0).astype(BF)
    partial = matmul(ordered, wo_ref[...]).astype(BF)
    keep_ref[...] = partial[: rows // 2]
    send_ref[...] = partial[rows // 2 :]

    slots = combine_ref.shape[1]
    column = iota((1, slots), 1)
    expert, slot = column // cap, column % cap
    hit0 = routes_ref[:, 0:1] == expert
    hit1 = routes_ref[:, 1:2] == expert
    rank = matmul(strict_lower(rows), (hit0 | hit1).astype(BF)).astype(jnp.int32)
    here = rank == slot
    weight = jnp.where(hit0 & here, rw_ref[:, 0:1], 0.0) + jnp.where(hit1 & here, rw_ref[:, 1:2], 0.0)
    combine_ref[...] = weight.astype(BF)
    for c in copies:
        c.wait()


def swapped_rows(value, cap, tp, bit):
    blocks = value.shape[0] // cap
    take = lambda i: value[(i ^ bit) * cap : (i ^ bit) * cap + cap]
    return jnp.concatenate([take(i) for i in range(blocks)], axis=0)


def expert_body(cap, order, place_ref, *refs):
    tp_index = place_ref[1]
    count = len(refs) - 8
    block_refs = refs[:count]
    wg_ref, wu_ref, wd_ref, send_ref, keep_ref, x_ref, h_ref, hs_ref = refs[count:]
    for i, block_ref in enumerate(block_refs):
        x_ref[i * cap : (i + 1) * cap, :] = block_ref[...]
    units = wg_ref.shape[1]
    tile = min(256, units)

    def hidden(i, _):
        at = pl.ds(pl.multiple_of(i * tile, tile), tile)
        x = x_ref[...]
        gate = matmul(x, wg_ref[:, at])
        up = matmul(x, wu_ref[:, at])
        value = gate / (1.0 + jnp.exp(-gate)) * up
        h_ref[:, at] = value.astype(BF)
        hs_ref[:, at] = swapped_rows(value, cap, len(order), 1).astype(BF)
        return 0

    lax.fori_loop(0, units // tile, hidden, 0)
    slice_width = wd_ref.shape[1] // len(order)
    kept = len(order) // 2
    width = min(256, slice_width)
    parts = slice_width // width
    for i, n in enumerate(order):
        base = (tp_index ^ n) * slice_width
        lhs_ref, out_ref = (h_ref, keep_ref) if i < kept else (hs_ref, send_ref)
        for j in range(parts):
            at = pl.ds(pl.multiple_of(base + j * width, width), width)
            column = (i % kept) * slice_width + j * width
            out_ref[:, column : column + width] = matmul(lhs_ref[...], wd_ref[:, at]).astype(BF)


def half_body(cap, tp, bit, keep_ref, got_ref, next_keep_ref, next_send_ref):
    middle = keep_ref.shape[1] // 2
    total = keep_ref[...].astype(F32) + got_ref[...].astype(F32)
    next_keep_ref[...] = total[:, :middle].astype(BF)
    next_send_ref[...] = swapped_rows(total[:, middle:], cap, tp, bit).astype(BF)


def last_body(cap, tp, place_ref, keep_ref, got_ref, out_ref):
    ep_index, tp_index = place_ref[0], place_ref[1]
    total = (keep_ref[...].astype(F32) + got_ref[...].astype(F32)).astype(BF)
    for i in range(total.shape[0] // cap):
        k, m = i // tp, i % tp
        out_ref[ep_index ^ (k * tp + (tp_index ^ m))] = total[i * cap : (i + 1) * cap]


def combine_body(combine_ref, rows_ref, out_ref):
    out_ref[...] = matmul(combine_ref[...], rows_ref[...]).astype(BF)


def halves_order(tp):
    bits = tp.bit_length() - 1
    return sorted(range(tp), key=lambda n: [n >> b & 1 for b in range(bits)])


def swap_pairs(count, bit):
    return [(i, i ^ bit) for i in range(count)]


def on_device(
    queries,
    key_states,
    value_states,
    sink_logit,
    out_weight,
    expert_input,
    norm_gain,
    routes,
    route_weight,
    gate_weight,
    up_weight,
    down_weight,
):
    ep, tp = lax.axis_size("ep"), lax.axis_size("tp")
    ep_index, tp_index = lax.axis_index("ep"), lax.axis_index("tp")
    rows, width = expert_input.shape
    local_heads = queries.shape[1] // HEAD_DIM
    group_size = HEADS // KV_HEADS
    expert_count = ep * gate_weight.shape[0]
    cap = rows * TOP * 5 // (4 * expert_count)
    slots = expert_count * cap
    hops = ep // tp
    order = halves_order(tp)
    units = gate_weight.shape[2]
    place = jnp.stack([ep_index, tp_index, tp_index * local_heads // group_size, ep]).astype(jnp.int32)
    block = jax.ShapeDtypeStruct((cap, width), BF)

    kv, *blocks = call(
        functools.partial(pack_body, cap, hops, tp),
        [jax.ShapeDtypeStruct((rows, 2 * HEAD_DIM), BF)] + [block] * hops,
        (place, expert_input, norm_gain.reshape(1, width), routes, key_states, value_states),
        [SM] + [VM] * 5,
        flops=2 * LANES * LANES * width,
        nbytes=rows * width * 2,
        name="pack",
    )

    held = {}
    for k in reversed(range(hops)):
        pairs = [(e * tp + t, (e ^ (k * tp + t)) * tp + t) for e in range(ep) for t in range(tp)]
        held[k, 0] = lax.ppermute(blocks[k], ("ep", "tp"), pairs)
    up_pairs = [(i, i + 1) for i in range(ep - 1)]
    down_pairs = [(i + 1, i) for i in range(ep - 1)]
    low = lax.ppermute(kv, "ep", up_pairs)
    high = lax.ppermute(kv, "ep", down_pairs)

    half = HEAD_DIM // 2
    frequency = jnp.power(F32(ROTARY_BASE), -(jnp.arange(half, dtype=F32) * (2.0 / HEAD_DIM)))
    span_pos = ep_index * rows - WINDOW + jnp.arange(rows + 2 * WINDOW, dtype=jnp.int32)
    angles = span_pos.astype(F32)[:, None] * frequency[None, :]
    cosine, sine = jnp.cos(angles), jnp.sin(angles)
    table = jnp.concatenate([cosine, cosine, -sine, sine], axis=1)

    gate_rows, up_rows, down_rows = gate_weight[0], up_weight[0], down_weight[0]
    shape = lambda a: jax.ShapeDtypeStruct(a.shape, a.dtype)
    half_rows = jax.ShapeDtypeStruct((rows // 2, width), BF)
    mix_send, mix_keep, combine, gate_v, up_v, down_v = call(
        functools.partial(mixer_body, cap, order),
        [half_rows, half_rows, jax.ShapeDtypeStruct((rows, slots), BF)]
        + [pltpu.VMEM(a.shape, a.dtype) for a in (gate_rows, up_rows, down_rows)],
        (place, queries, kv, low, high, table, sink_logit, routes, route_weight, out_weight, gate_rows, up_rows, down_rows),
        [SM] + [VM] * 5 + [SM] + [VM] * 3 + [ANY] * 3,
        scratch=[pltpu.VMEM((rows, local_heads * HEAD_DIM), F32), pltpu.SemaphoreType.DMA((3,))],
        flops=4 * rows * width * local_heads * HEAD_DIM,
        nbytes=3 * units * width * 2,
        limit=36,
        name="mixer",
    )

    bit = tp // 2
    while bit:
        for k in reversed(range(hops)):
            for m in [m for kk, m in held if kk == k]:
                held[k, m ^ bit] = lax.ppermute(held[k, m], "tp", swap_pairs(tp, bit))
        bit //= 2

    send, keep = call(
        functools.partial(expert_body, cap, order),
        [jax.ShapeDtypeStruct((slots, width // 2), BF)] * 2,
        (place, *[held[k, m] for k in range(hops) for m in range(tp)], gate_v, up_v, down_v),
        [SM] + [VM] * (hops * tp + 3),
        scratch=[pltpu.VMEM((slots, width), BF), pltpu.VMEM((slots, units), BF), pltpu.VMEM((slots, units), BF)],
        flops=6 * slots * width * units,
        nbytes=slots * width * 4,
        limit=36,
        name="expert",
    )

    bit = 1
    while bit < tp:
        got = lax.ppermute(send, "tp", swap_pairs(tp, bit))
        mix_got = lax.ppermute(mix_send, "tp", swap_pairs(tp, bit))
        mix = (mix_keep.astype(F32) + mix_got.astype(F32)).astype(BF)
        if bit * 2 < tp:
            middle = keep.shape[1] // 2
            keep, send = call(
                functools.partial(half_body, cap, tp, bit * 2),
                [jax.ShapeDtypeStruct((slots, middle), BF)] * 2,
                (keep, got),
                [VM] * 2,
                flops=slots * middle,
                nbytes=slots * middle * 8,
                name="half",
            )
            mix_keep, mix_send = mix[: mix.shape[0] // 2], mix[mix.shape[0] // 2 :]
        bit *= 2
    (ready,) = call(
        functools.partial(last_body, cap, tp),
        [jax.ShapeDtypeStruct((ep, cap, width // tp), BF)],
        (place, keep, got),
        [SM, VM, VM],
        flops=slots * width // tp,
        nbytes=slots * width // tp * 6,
        name="last",
    )
    returned = lax.all_to_all(ready, "ep", split_axis=0, concat_axis=0, tiled=True)
    (expert_out,) = call(
        combine_body,
        [jax.ShapeDtypeStruct((rows, width // tp), BF)],
        (combine, returned.reshape(slots, width // tp)),
        [VM, VM],
        flops=2 * slots * rows * width // tp,
        nbytes=slots * width // tp * 2,
        name="combine",
    )
    return (mix, expert_out)


def solution(mesh):
    in_specs = (
        P("ep", "tp"),
        P("ep", None),
        P("ep", None),
        P("tp"),
        P("tp", None),
        P("ep", None),
        P(),
        P("ep", None),
        P("ep", None),
        P("ep", None, "tp"),
        P("ep", None, "tp"),
        P("ep", "tp", None),
    )
    out_specs = (P(("ep", "tp"), None), P("ep", "tp"))
    return jax.shard_map(
        on_device, mesh=mesh, in_specs=in_specs, out_specs=out_specs, check_vma=False
    )
```
